32 devices in a mesh: grp: 2 (over y), ep: 8 (over z, x), tp: 2 (over core).
Axes of the slice: x: 2, y: 2, z: 4, core: 2. Of those that a mesh axis runs over, the one named last changes fastest.
Arguments:
- tokens: bfloat16 [2048, 2048], P(('grp', 'ep')), parts along dimension 0, may hold values from -6 to 6
- in_gain: float32 [2048], replicated, may hold values from 0.1 to 1.9
- routing: int32 [2048, 4], P(('grp', 'ep')), parts along dimension 0, may hold values from 0 to 15, as said below
- gate_prob: float32 [2048, 4], P(('grp', 'ep')), parts along dimension 0, may hold values from 0.05 to 1
- w_gate: bfloat16 [16, 2048, 512], P('ep', None, 'tp'), may hold values from -0.125 to 0.125
- w_up: bfloat16 [16, 2048, 512], P('ep', None, 'tp'), may hold values from -0.125 to 0.125
- w_down: bfloat16 [16, 512, 2048], P('ep', 'tp')
- out_gain: float32 [2048], P('tp'), may hold values from 0.1 to 1.9
Outputs:
- output: bfloat16 [2048, 2048], P(('grp', 'ep'), 'tp'), parts along dimension 0
The draws below stay inside these ranges and needn't reach their ends.
There are 2 independent parts, one for each index of `grp`. The reference program is written for one: setup_inputs(seed, part) draws one part's arguments, and reference() takes and returns one part's arrays. A program takes and returns all parts, laid end to end along the dimension named above; an argument that names none is the same for every part. Nothing has to cross between parts.
Inputs may be any that keep to these rules, and one draw needn't show every extreme that they name: `routing`: each row names 4 different experts, all of one group (the same value of expert // 4). In the rows of one device no expert is named more than 64 times, and in every device's rows some expert is named exactly 64 times.
All inputs are finite; a program needn't handle non-finite values.
Results may differ from the reference program's by a relative error of at most 0.0077.
Values may be sent and summed in bfloat16 or wider, within the bound.
A program may use at most 64 MiB of HBM per device.

```python
import math
import jax
import jax.numpy as jnp
from jax import lax

D = 2048
FF = 512
GROUPS = 4
TOPK = 4
TOK_DEV = 128
EXPERTS = 16
EPG = 4
TOKENS = 1024
CAP = 64
GMAX = 64
N_EP = 8
N_TP = 2


def draw_routing(key, part):
    block_count = TOKENS // TOK_DEV
    key_order, key_pick, key_perm, key_shuffle = jax.random.split(key, 4)
    hot_count = min(GMAX, TOK_DEV)
    hot_span = hot_count * TOPK // CAP
    group_order = jax.random.permutation(key_order, GROUPS)
    hot_picks = jnp.minimum(jax.random.randint(key_pick, (block_count,), 0, GROUPS + 2), GROUPS - 1)
    hot_group = group_order[hot_picks]
    position = jnp.arange(TOK_DEV, dtype=jnp.int32)
    is_hot = position < hot_count
    cold_index = position - hot_count
    groups = jnp.where(is_hot[None, :], hot_group[:, None], (hot_group[:, None] + 1 + cold_index[None, :] % (GROUPS - 1)) % GROUPS)
    group_rank = jnp.where(is_hot, position, cold_index // (GROUPS - 1))
    modulus = jnp.where(is_hot, hot_span, EPG)
    within = (group_rank[:, None] * TOPK + jnp.arange(TOPK, dtype=jnp.int32)[None, :]) % modulus[:, None]
    perm_keys = jax.random.split(key_perm, block_count * GROUPS)
    orders = jax.vmap(lambda one_key: jax.random.permutation(one_key, EPG))(perm_keys).reshape(block_count, GROUPS, EPG)
    block_ids = jnp.arange(block_count)[:, None, None]
    local_ids = orders[block_ids, groups[:, :, None], within[None, :, :]]
    experts = groups[:, :, None] * EPG + local_ids
    shuffle_keys = jax.random.split(key_shuffle, block_count)
    shuffles = jax.vmap(lambda one_key: jax.random.permutation(one_key, TOK_DEV))(shuffle_keys)
    experts = jnp.take_along_axis(experts, shuffles[:, :, None], axis=1)
    return experts.reshape(TOKENS, TOPK).astype(jnp.int32)


def draw_w_down(key, part):
    key_base, key_col = jax.random.split(key)
    columns = jnp.arange(D, dtype=jnp.float32) / D
    entries_base = jax.random.normal(key_base, (EXPERTS, FF, D), jnp.float32)
    spread = jax.random.uniform(key_col, (D,), jnp.float32, 0.5, 1.5)
    col_rise = 3.0 ** columns
    return (entries_base * FF ** (-0.5) * col_rise * spread).astype(jnp.bfloat16)


def levels(own_key, dims, cuts, low, largest):
    def one(dim, parts):
        draws = jax.random.uniform(jax.random.fold_in(jax.random.fold_in(own_key, 6), dim), (parts,), jnp.float32, low / len(cuts), largest / len(cuts))
        return jnp.repeat(jnp.exp(draws), dims[dim] // parts).reshape((-1,) + (1,) * (len(dims) - dim - 1))

    gain = one(*cuts[0])
    for cut in cuts[1:]:
        gain = gain * one(*cut)
    return gain


def bell_draw(rng, extent, width, most, cuts=(), kind=jnp.bfloat16):
    result = jax.random.normal(rng, extent, jnp.float32) * width
    if len(cuts) > 0:
        result = levels(rng, extent, cuts, -0.22, 0.18) * result
    return jnp.clip(result, min=-most, max=most).astype(kind)


def setup_inputs(seed: int = 0, part: int = 0) -> dict:
    seeds = jax.random.split(jax.random.key(seed), 9)
    part_keys = jax.random.split(jax.random.fold_in(seeds[8], part), 9)
    tokens = bell_draw(part_keys[0], (TOKENS, D), 1.0, 6.0, ((0, 8),))
    in_gain = jnp.clip(1.0 + 0.18 * jax.random.normal(seeds[1], (D,), jnp.float32), 0.1, 1.9)
    routing = draw_routing(jax.random.fold_in(jax.random.fold_in(seeds[8], part), 71), part)
    gate_prob = jnp.clip(jnp.exp(math.log(1.0) - 2.9957323 * jax.random.uniform(part_keys[3], (TOKENS, TOPK), jnp.float32) ** levels(part_keys[3], (TOKENS, TOPK), ((0, 8),), -0.2, 0.2)), 0.05, 1.0)
    w_gate = bell_draw(seeds[4], (EXPERTS, D, FF), D ** -0.5, 0.125, ((0, 8), (2, 2)))
    w_up = bell_draw(seeds[5], (EXPERTS, D, FF), D ** -0.5, 0.125, ((0, 8), (2, 2)))
    w_down = draw_w_down(jax.random.fold_in(seeds[8], 71), part)
    out_gain = jnp.clip(1.0 + 0.18 * jax.random.normal(seeds[7], (D,), jnp.float32), 0.1, 1.9)
    return dict(tokens=tokens, in_gain=in_gain, routing=routing, gate_prob=gate_prob, w_gate=w_gate, w_up=w_up, w_down=w_down, out_gain=out_gain)


EPS = 1e-06

def slot_ranks(flat_routes):
    matches = (flat_routes[:, None] == jnp.arange(EXPERTS, dtype=jnp.int32)[None, :]).astype(jnp.int32)
    earlier = jnp.cumsum(matches, axis=0) - matches
    return lax.optimization_barrier(jnp.sum(earlier * matches, axis=1)).astype(jnp.int32)

def reference(tokens, in_gain, routing, gate_prob, w_gate, w_up, w_down, out_gain):
    floats = tokens.astype(jnp.float32)
    normed = (floats * lax.rsqrt(lax.optimization_barrier(jnp.mean(floats * floats, axis=-1, keepdims=True)) + EPS) * in_gain).astype(jnp.bfloat16)
    blocks = routing.reshape(N_EP, TOK_DEV * TOPK)
    slot_rank = jax.vmap(slot_ranks)(blocks)
    sources = jnp.arange(N_EP, dtype=jnp.int32)[:, None]
    slot_ids = (blocks * (N_EP * CAP) + sources * CAP + slot_rank).reshape(-1).astype(jnp.int32)
    token_ids = jnp.arange(TOKENS * TOPK, dtype=jnp.int32) // TOPK
    slot_table = jnp.zeros((EXPERTS * N_EP * CAP,), jnp.int32).at[slot_ids].set(token_ids + 1)
    slot_table = slot_table.reshape(EXPERTS, N_EP * CAP)

    def expert(inputs):
        entries, gate_w, up_w, down_w = inputs
        filled = entries > 0
        rows_in = jnp.where(filled[:, None], normed[jnp.maximum(entries - 1, 0)], jnp.zeros((), jnp.bfloat16))
        gate_act = jnp.dot(rows_in, gate_w, preferred_element_type=jnp.float32)
        up_act = jnp.dot(rows_in, up_w, preferred_element_type=jnp.float32)
        hidden = (jax.nn.silu(gate_act) * up_act).astype(jnp.bfloat16)
        pieces = jnp.einsum('rnf,nfd->nrd', hidden.reshape(-1, N_TP, FF // N_TP).astype(jnp.float32), down_w.reshape(N_TP, FF // N_TP, D).astype(jnp.float32))
        rounded = lax.optimization_barrier(pieces.astype(jnp.bfloat16))
        return lax.optimization_barrier(jnp.sum(rounded.astype(jnp.float32), axis=0)).astype(jnp.bfloat16)
    results = lax.map(expert, (slot_table, w_gate, w_up, w_down))
    picked = results.reshape(-1, D)[slot_ids].astype(jnp.float32).reshape(TOKENS, TOPK, D)
    mixed_rows = lax.optimization_barrier(jnp.sum(picked * gate_prob[:, :, None], axis=1))
    inv_rms = lax.rsqrt(lax.optimization_barrier(jnp.mean(mixed_rows * mixed_rows, axis=-1, keepdims=True)) + EPS)
    return (mixed_rows * inv_rms * out_gain).astype(jnp.bfloat16)
```

```python
import functools

import jax
import jax.numpy as jnp
from jax import lax
from jax.experimental import pallas as pl
from jax.experimental.pallas import tpu as pltpu
from jax.sharding import PartitionSpec as P

GROUPS = 4
EPS = 1e-06
MESH = pl.DeviceIdType.MESH
F32 = jnp.float32
BF16 = jnp.bfloat16


def loop(low, high, step):
    if high - low <= 8:
        for i in range(low, high):
            step(i)
    else:
        lax.fori_loop(low, high, lambda i, carry: (step(i), carry)[1], 0)


def kernel(
    group_count, span, rows,
    routes_ref, probs_ref, in_gain_ref, out_gain_ref, tokens_ref, gate_hbm, up_hbm, down_hbm,
    out_ref,
    sendz, gathered, unpack, gate_send, gate_recv, w_gate, w_up, w_down, hidden,
    kept, tp_send, tp_recv, own_sum, grp_recv, home_send, home_recv, sq_send, sq_recv,
    w_sem, gate_ss, gate_rs, z_ss, z_rs, x_ss, x_rs, t_ss, t_rs, p_ss, p_rs, r_ss, r_rs, h_ss, h_rs, q_ss, q_rs,
):
    Q, S, R = group_count, span, rows
    N = Q * S
    top, tok = routes_ref.shape
    width = tokens_ref.shape[1]
    H = out_ref.shape[1]
    L, _, F = gate_hbm.shape
    group_width = S * L
    gate_rows, lanes = gate_send.shape[1:]
    me = lax.axis_index("ep")
    c = lax.axis_index("tp")
    q, s = me // S, lax.rem(me, S)
    order = [0] + sorted(range(1, Q), key=lambda d: -min(d, Q - d))

    def at(ep, tp=None):
        return {"ep": ep, "tp": c if tp is None else tp}

    def remote(src, dst, ss, rs, dev):
        return pltpu.make_async_remote_copy(
            src_ref=src, dst_ref=dst, send_sem=ss, recv_sem=rs, device_id=dev, device_id_type=MESH
        )

    barrier = pltpu.get_barrier_semaphore()
    loop(1, N, lambda p: pl.semaphore_signal(
        barrier, inc=1, device_id=at(lax.rem(me + p, N)), device_id_type=MESH))
    pl.semaphore_signal(barrier, inc=1, device_id=at(me, 1 - c), device_id_type=MESH)

    weights = []
    for n, (src, dst) in enumerate(((gate_hbm, w_gate), (up_hbm, w_up), (down_hbm, w_down))):
        for e in range(L):
            weights.append(pltpu.make_async_copy(src.at[e], dst.at[e], w_sem.at[n, e]))
    for copy in weights:
        copy.start()

    floats = tokens_ref[...].astype(F32)
    inv = lax.rsqrt(jnp.mean(floats * floats, axis=-1, keepdims=True) + EPS)
    own_cols = pl.ds(pl.multiple_of(c * H, H), H)
    other_cols = pl.ds(pl.multiple_of((1 - c) * H, H), H)
    normed = (tokens_ref[:, own_cols].astype(F32) * inv * in_gain_ref[:, own_cols]).astype(BF16)
    first = routes_ref[0:1, :]
    groups = lax.broadcasted_iota(jnp.int32, (16, tok), 0)
    member = (first >= groups * group_width) & (first < (groups + 1) * group_width)
    earlier = lax.broadcasted_iota(jnp.int32, (tok, tok), 0) < lax.broadcasted_iota(jnp.int32, (tok, tok), 1)
    rank = jnp.dot(
        jnp.where(member, 1.0, 0.0).astype(BF16), jnp.where(earlier, 1.0, 0.0).astype(BF16),
        preferred_element_type=F32,
    ).astype(jnp.int32)
    slots = lax.broadcasted_iota(jnp.int32, (lanes, tok), 0)
    picks = []
    for g in range(Q):
        inside = (first >= g * group_width) & (first < (g + 1) * group_width)
        picks.append(jnp.where((rank[g:g + 1, :] == slots) & inside, 1.0, 0.0))
        sendz[g] = jnp.dot(
            picks[g][:R].astype(BF16), normed, preferred_element_type=F32
        ).astype(BF16)

    gathered[q, s, c] = sendz[q]
    pl.semaphore_wait(barrier, N)

    def z_copy(d):
        to = lax.rem(q + d, Q)
        return remote(sendz.at[to], gathered.at[q, s, c], z_ss.at[d], z_rs.at[d], at(to * S + s))

    def source(d):
        return lax.rem(q + Q - d, Q)

    def x_copy(d, e):
        block = gathered.at[source(d), s, c]
        return remote(block, block, x_ss.at[d, e], x_rs.at[d, e], at(q * S + lax.rem(s + e, S)))

    def t_copy(d, e):
        block = gathered.at[source(d), lax.rem(s + S - e, S), c]
        return remote(block, block, t_ss.at[d, e], t_rs.at[d, e], at(me, 1 - c))

    def gate_copy(p):
        to = lax.rem(me + p, N)
        return remote(gate_send.at[to // S], gate_recv.at[me], gate_ss.at[p], gate_rs.at[p], at(to))

    def p_copy(d):
        return remote(tp_send.at[d], tp_recv.at[d], p_ss.at[d], p_rs.at[d], at(me, 1 - c))

    def r_copy(d, e):
        to = lax.rem(s + e, S)
        return remote(tp_send.at[d, to], grp_recv.at[d, e], r_ss.at[d, e], r_rs.at[d, e], at(q * S + to))

    def h_copy(d):
        return remote(home_send.at[d], home_recv.at[q], h_ss.at[d], h_rs.at[d], at(source(d) * S + s))

    def forward(d):
        loop(1, S, lambda e: x_copy(d, e).start())
        t_copy(d, 0).start()

    for d in order[1:]:
        z_copy(d).start()
    forward(0)

    for g in range(Q):
        ids = g * group_width + lax.broadcasted_iota(jnp.int32, (gate_rows, tok), 0)
        dense = jnp.zeros((gate_rows, tok), F32)
        for k in range(top):
            dense += jnp.where(routes_ref[k:k + 1, :] == ids, probs_ref[k:k + 1, :], 0.0)
        gate_send[g] = lax.dot_general(
            dense, picks[g], (((1,), (1,)), ((), ())),
            precision=lax.Precision.HIGHEST, preferred_element_type=F32,
        )
    gate_recv[me] = gate_send[q]
    loop(1, N, lambda p: gate_copy(p).start())
    unpack[...] = jnp.concatenate([pick[:R] for pick in picks], axis=0).T.astype(BF16)

    def stage_a(d):
        z_copy(d).wait_recv()
        forward(d)

    def stage_b(d):
        def one(e):
            x_copy(d, e).wait_recv()
            t_copy(d, e).start()
        loop(1, S, one)

    pair = 2 if S % 2 == 0 else 1

    def stage_c(d):
        loop(0, S, lambda e: t_copy(d, e).wait_recv())
        src = source(d)
        diagonal = (
            lax.broadcasted_iota(jnp.int32, (R, lanes), 0) == lax.broadcasted_iota(jnp.int32, (R, lanes), 1)
        )

        def some(n):
            base = n * pair
            low = gathered[src, pl.ds(base, pair), 0].reshape(pair * R, H)
            high = gathered[src, pl.ds(base, pair), 1].reshape(pair * R, H)
            for j in range(L):
                gate = jnp.dot(low, w_gate[j, :H], preferred_element_type=F32)
                gate += jnp.dot(high, w_gate[j, H:], preferred_element_type=F32)
                up = jnp.dot(low, w_up[j, :H], preferred_element_type=F32)
                up += jnp.dot(high, w_up[j, H:], preferred_element_type=F32)
                scales = []
                for b in range(pair):
                    line = gate_recv[src * S + base + b, pl.ds(s * L + j, 1), :]
                    scales.append(jnp.sum(jnp.where(diagonal, line, 0.0), axis=1, keepdims=True))
                scale = jnp.concatenate(scales, axis=0)
                act = gate / (1.0 + jnp.exp(-gate)) * up
                hidden[:, j * F:(j + 1) * F] = (act * scale).astype(BF16)
            other = jnp.zeros((pair * R, H), F32)
            mine = jnp.zeros((pair * R, H), F32)
            for j in range(L):
                other += jnp.dot(hidden[:, j * F:(j + 1) * F], w_down[j, :, other_cols], preferred_element_type=F32)
            tp_send[d, pl.ds(base, pair)] = other.astype(BF16).reshape(pair, R, H)
            for j in range(L):
                mine += jnp.dot(hidden[:, j * F:(j + 1) * F], w_down[j, :, own_cols], preferred_element_type=F32)
            kept[pl.ds(base, pair)] = mine.reshape(pair, R, H)

        if S == pair:
            some(0)
        else:
            lax.fori_loop(0, S // pair, lambda n, carry: (some(n), carry)[1], 0)
        p_copy(d).start()

    def stage_e(d):
        p_copy(d).wait()
        def one(e):
            to = lax.rem(s + e, S)
            tp_send[d, to] = (kept[to] + tp_recv[d, to].astype(F32)).astype(BF16)
            r_copy(d, e).start()
        loop(1, S, one)
        own_sum[...] = kept[s] + tp_recv[d, s].astype(F32)

    def stage_f(d):
        def one(e):
            r_copy(d, e).wait_recv()
            own_sum[...] += grp_recv[d, e].astype(F32)
        loop(1, S, one)
        if d == 0:
            home_recv[q] = own_sum[...].astype(BF16)
        else:
            home_send[d] = own_sum[...].astype(BF16)
            h_copy(d).start()

    stage_b(0)
    for i in range(Q):
        if i + 1 < Q:
            stage_a(order[i + 1])
        if i == 0:
            loop(1, N, lambda p: gate_copy(p).wait_recv())
            for copy in weights:
                copy.wait()
        if i >= 1:
            if i >= 2:
                stage_f(order[i - 2])
            stage_e(order[i - 1])
        stage_c(order[i])
        if i + 1 < Q:
            stage_b(order[i + 1])
    if Q >= 2:
        stage_f(order[Q - 2])
    stage_e(order[Q - 1])
    stage_f(order[Q - 1])

    for d in order[1:]:
        h_copy(d).wait_recv()
    mixed = jnp.dot(unpack[...], home_recv[...].reshape(Q * R, H), preferred_element_type=F32)
    squares = jnp.sum(mixed * mixed, axis=1, keepdims=True)
    sq_send[...] = jnp.broadcast_to(squares, sq_send.shape)
    sq_copy = remote(sq_send, sq_recv, q_ss, q_rs, at(me, 1 - c))
    sq_copy.start()
    for d in range(1, Q):
        z_copy(d).wait_send()
        h_copy(d).wait_send()
    for d in range(Q):
        def sent(e):
            x_copy(d, e).wait_send()
            r_copy(d, e).wait_send()
        loop(1, S, sent)
        loop(0, S, lambda e: t_copy(d, e).wait_send())
    loop(1, N, lambda p: gate_copy(p).wait_send())
    sq_copy.wait()
    total = squares + sq_recv[:, 0:1]
    out_ref[...] = (mixed * lax.rsqrt(total / width + EPS) * out_gain_ref[...]).astype(BF16)


def body(tokens, in_gain, routing, gate_prob, w_gate, w_up, w_down, out_gain):
    N = lax.axis_size("ep")
    L, D, F = w_gate.shape
    tok, top = routing.shape
    H = out_gain.shape[0]
    group_width = L * N // GROUPS
    cap = max(2, tok * top // (2 * group_width))
    R = min(tok, group_width * cap // top)
    R = -(-R // 16) * 16
    Q, S = GROUPS, N // GROUPS
    lanes = -(-R // 128) * 128
    gate_rows = -(-group_width // 8) * 8
    pair = 2 if S % 2 == 0 else 1
    vmem = pl.BlockSpec(memory_space=pltpu.VMEM)
    hbm = pl.BlockSpec(memory_space=pl.ANY)
    dma = pltpu.SemaphoreType.DMA
    return pl.pallas_call(
        functools.partial(kernel, Q, S, R),
        out_shape=jax.ShapeDtypeStruct((tok, H), BF16),
        in_specs=[vmem] * 5 + [hbm] * 3,
        out_specs=vmem,
        scratch_shapes=[
            pltpu.VMEM((Q, R, H), BF16),
            pltpu.VMEM((Q, S, 2, R, H), BF16),
            pltpu.VMEM((tok, Q * R), BF16),
            pltpu.VMEM((Q, gate_rows, lanes), F32),
            pltpu.VMEM((N, gate_rows, lanes), F32),
            pltpu.VMEM((L, D, F), BF16),
            pltpu.VMEM((L, D, F), BF16),
            pltpu.VMEM((L, F, D), BF16),
            pltpu.VMEM((pair * R, L * F), BF16),
            pltpu.VMEM((S, R, H), F32),
            pltpu.VMEM((Q, S, R, H), BF16),
            pltpu.VMEM((Q, S, R, H), BF16),
            pltpu.VMEM((R, H), F32),
            pltpu.VMEM((Q, S, R, H), BF16),
            pltpu.VMEM((Q, R, H), BF16),
            pltpu.VMEM((Q, R, H), BF16),
            pltpu.VMEM((tok, 128), F32),
            pltpu.VMEM((tok, 128), F32),
            dma((3, L)), dma((N,)), dma((N,)), dma((Q,)), dma((Q,)),
            dma((Q, S)), dma((Q, S)), dma((Q, S)), dma((Q, S)),
            dma((Q,)), dma((Q,)), dma((Q, S)), dma((Q, S)), dma((Q,)), dma((Q,)),
            dma, dma,
        ],
        compiler_params=pltpu.CompilerParams(
            collective_id=0, has_side_effects=True, vmem_limit_bytes=64 * 1000 * 1000
        ),
    )(routing.T, gate_prob.T, in_gain.reshape(1, D), out_gain.reshape(1, H), tokens, w_gate, w_up, w_down)


def solution(mesh):
    placed = (
        P(("grp", "ep"), None),
        P(),
        P(("grp", "ep"), None),
        P(("grp", "ep"), None),
        P("ep", None, "tp"),
        P("ep", None, "tp"),
        P("ep", "tp", None),
        P("tp"),
    )
    return jax.shard_map(
        body, mesh=mesh, in_specs=placed, out_specs=P(("grp", "ep"), "tp"), check_vma=False
    )
```

```python
import functools

import jax
import jax.numpy as jnp
from jax import lax
from jax.experimental import pallas as pl
from jax.experimental.pallas import tpu as pltpu
from jax.sharding import PartitionSpec as P

GROUPS = 4
EPS = 1e-06
CHUNKS = 2
MESH = pl.DeviceIdType.MESH
F32 = jnp.float32
BF16 = jnp.bfloat16


def loop(low, high, step):
    if high - low <= 8:
        for i in range(low, high):
            step(i)
    else:
        lax.fori_loop(low, high, lambda i, carry: (step(i), carry)[1], 0)


def kernel(
    group_count, span, rows,
    routes_ref, probs_ref, in_gain_ref, out_gain_ref, tokens_hbm, gate_hbm, up_hbm, down_hbm,
    out_ref,
    tokens_ref, sendz, gathered, unpack, gate_send, gate_recv, w_gate, w_up, w_down, hidden,
    kept, tp_send, tp_recv, own_sum, grp_recv, home_send, home_recv, sq_send, sq_recv,
    tok_sem, w_sem, gate_ss, gate_rs, z_ss, z_rs, x_ss, x_rs, t_ss, t_rs, p_ss, p_rs, r_ss, r_rs, h_ss, h_rs, q_ss, q_rs,
):
    Q, S, R = group_count, span, rows
    N = Q * S
    K = CHUNKS
    RC = R // K
    top, tok = routes_ref.shape
    width = tokens_ref.shape[1]
    H = out_ref.shape[1]
    L, _, F = gate_hbm.shape
    group_width = S * L
    gate_rows, lanes = gate_send.shape[1:]
    me = lax.axis_index("ep")
    c = lax.axis_index("tp")
    q, s = me // S, lax.rem(me, S)
    order = [0] + sorted(range(1, Q), key=lambda d: -min(d, Q - d))

    def at(ep, tp=None):
        return {"ep": ep, "tp": c if tp is None else tp}

    def remote(src, dst, ss, rs, dev):
        return pltpu.make_async_remote_copy(
            src_ref=src, dst_ref=dst, send_sem=ss, recv_sem=rs, device_id=dev, device_id_type=MESH
        )

    tok_copy = pltpu.make_async_copy(tokens_hbm, tokens_ref, tok_sem)
    tok_copy.start()

    barrier = pltpu.get_barrier_semaphore()
    loop(1, N, lambda p: pl.semaphore_signal(
        barrier, inc=1, device_id=at(lax.rem(me + p, N)), device_id_type=MESH))
    pl.semaphore_signal(barrier, inc=1, device_id=at(me, 1 - c), device_id_type=MESH)

    weights = []
    for n, (src, dst) in enumerate(((gate_hbm, w_gate), (up_hbm, w_up), (down_hbm, w_down))):
        for e in range(L):
            weights.append(pltpu.make_async_copy(src.at[e], dst.at[e], w_sem.at[n, e]))
    for copy in weights:
        copy.start()

    first = routes_ref[0:1, :]
    groups = lax.broadcasted_iota(jnp.int32, (16, tok), 0)
    member = (first >= groups * group_width) & (first < (groups + 1) * group_width)
    earlier = lax.broadcasted_iota(jnp.int32, (tok, tok), 0) < lax.broadcasted_iota(jnp.int32, (tok, tok), 1)
    rank = jnp.dot(
        jnp.where(member, 1.0, 0.0).astype(BF16), jnp.where(earlier, 1.0, 0.0).astype(BF16),
        preferred_element_type=F32,
    ).astype(jnp.int32)
    slots = lax.broadcasted_iota(jnp.int32, (lanes, tok), 0)
    picks = []
    for g in range(Q):
        inside = (first >= g * group_width) & (first < (g + 1) * group_width)
        picks.append(jnp.where((rank[g:g + 1, :] == slots) & inside, 1.0, 0.0))

    tok_copy.wait()
    floats = tokens_ref[...].astype(F32)
    inv = lax.rsqrt(jnp.mean(floats * floats, axis=-1, keepdims=True) + EPS)
    own_cols = pl.ds(pl.multiple_of(c * H, H), H)
    other_cols = pl.ds(pl.multiple_of((1 - c) * H, H), H)
    normed = (tokens_ref[:, own_cols].astype(F32) * inv * in_gain_ref[:, own_cols]).astype(BF16)
    for g in range(Q):
        sendz[g] = jnp.dot(
            picks[g][:R].astype(BF16), normed, preferred_element_type=F32
        ).astype(BF16)

    gathered[q, s, c] = sendz[q]
    pl.semaphore_wait(barrier, N)

    def z_copy(d, k):
        to = lax.rem(q + d, Q)
        part = pl.ds(k * RC, RC)
        return remote(
            sendz.at[to, part], gathered.at[q, s, c, part], z_ss.at[d, k], z_rs.at[d, k], at(to * S + s)
        )

    def source(d):
        return lax.rem(q + Q - d, Q)

    def x_copy(d, e, k):
        block = gathered.at[source(d), s, c, pl.ds(k * RC, RC)]
        return remote(block, block, x_ss.at[d, e, k], x_rs.at[d, e, k], at(q * S + lax.rem(s + e, S)))

    def t_copy(d, e, k):
        block = gathered.at[source(d), lax.rem(s + S - e, S), c, pl.ds(k * RC, RC)]
        return remote(block, block, t_ss.at[d, e, k], t_rs.at[d, e, k], at(me, 1 - c))

    def gate_copy(d, e):
        to_q, to_s = lax.rem(q + d, Q), lax.rem(s + e, S)
        return remote(
            gate_send.at[to_q], gate_recv.at[me], gate_ss.at[d, e], gate_rs.at[d, e], at(to_q * S + to_s)
        )

    def p_copy(d):
        return remote(tp_send.at[d], tp_recv.at[d], p_ss.at[d], p_rs.at[d], at(me, 1 - c))

    def r_copy(d, e, k):
        to = lax.rem(s + e, S)
        part = pl.ds(k * RC, RC)
        return remote(
            tp_send.at[d, to, part], grp_recv.at[d, e, part], r_ss.at[d, e, k], r_rs.at[d, e, k], at(q * S + to)
        )

    def h_copy(d, k):
        part = pl.ds(k * RC, RC)
        return remote(
            home_send.at[d, part], home_recv.at[q, part], h_ss.at[d, k], h_rs.at[d, k], at(source(d) * S + s)
        )

    def forward(d, k):
        loop(1, S, lambda e: x_copy(d, e, k).start())
        t_copy(d, 0, k).start()

    for k in range(K):
        forward(0, k)
    for k in range(K):
        z_copy(order[1], k).start()

    for g in range(Q):
        ids = g * group_width + lax.broadcasted_iota(jnp.int32, (gate_rows, tok), 0)
        dense = jnp.zeros((gate_rows, tok), F32)
        for k in range(top):
            dense += jnp.where(routes_ref[k:k + 1, :] == ids, probs_ref[k:k + 1, :], 0.0)
        gate_send[g] = lax.dot_general(
            dense, picks[g], (((1,), (1,)), ((), ())),
            precision=lax.Precision.HIGHEST, preferred_element_type=F32,
        )
    gate_recv[me] = gate_send[q]

    for d in order:
        loop(1 if d == 0 else 0, S, lambda e: gate_copy(d, e).start())
    for d in order[2:]:
        for k in range(K):
            z_copy(d, k).start()

    unpack[...] = jnp.concatenate([pick[:R] for pick in picks], axis=0).T.astype(BF16)

    def stage_a(d):
        for k in range(K):
            z_copy(d, k).wait_recv()
            forward(d, k)

    def stage_b(d):
        for k in range(K):
            def one(e):
                x_copy(d, e, k).wait_recv()
                t_copy(d, e, k).start()
            loop(1, S, one)

    pair = 2 if S % 2 == 0 else 1

    def stage_c(d):
        loop(1 if d == 0 else 0, S, lambda e: gate_copy(d, e).wait_recv())
        for k in range(K):
            loop(0, S, lambda e: t_copy(d, e, k).wait_recv())
        src = source(d)
        diagonal = (
            lax.broadcasted_iota(jnp.int32, (R, lanes), 0) == lax.broadcasted_iota(jnp.int32, (R, lanes), 1)
        )

        def some(n):
            base = n * pair
            low = gathered[src, pl.ds(base, pair), 0].reshape(pair * R, H)
            high = gathered[src, pl.ds(base, pair), 1].reshape(pair * R, H)
            for j in range(L):
                gate = jnp.dot(low, w_gate[j, :H], preferred_element_type=F32)
                gate += jnp.dot(high, w_gate[j, H:], preferred_element_type=F32)
                up = jnp.dot(low, w_up[j, :H], preferred_element_type=F32)
                up += jnp.dot(high, w_up[j, H:], preferred_element_type=F32)
                scales = []
                for b in range(pair):
                    line = gate_recv[src * S + base + b, pl.ds(s * L + j, 1), :]
                    scales.append(jnp.sum(jnp.where(diagonal, line, 0.0), axis=1, keepdims=True))
                scale = jnp.concatenate(scales, axis=0)
                act = gate / (1.0 + jnp.exp(-gate)) * up
                hidden[:, j * F:(j + 1) * F] = (act * scale).astype(BF16)
            other = jnp.zeros((pair * R, H), F32)
            mine = jnp.zeros((pair * R, H), F32)
            for j in range(L):
                other += jnp.dot(hidden[:, j * F:(j + 1) * F], w_down[j, :, other_cols], preferred_element_type=F32)
            tp_send[d, pl.ds(base, pair)] = other.astype(BF16).reshape(pair, R, H)
            for j in range(L):
                mine += jnp.dot(hidden[:, j * F:(j + 1) * F], w_down[j, :, own_cols], preferred_element_type=F32)
            kept[min(d, 1), pl.ds(base, pair)] = mine.reshape(pair, R, H)

        if S == pair:
            some(0)
        else:
            lax.fori_loop(0, S // pair, lambda n, carry: (some(n), carry)[1], 0)
        p_copy(d).start()

    def stage_e(d):
        p_copy(d).wait()
        for k in range(K):
            part = pl.ds(k * RC, RC)

            def one(e):
                to = lax.rem(s + e, S)
                tp_send[d, to, part] = (kept[min(d, 1), to, part] + tp_recv[d, to, part].astype(F32)).astype(BF16)
                r_copy(d, e, k).start()
            loop(1, S, one)
        own_sum[d] = kept[min(d, 1), s] + tp_recv[d, s].astype(F32)

    def stage_f(d):
        for k in range(K):
            part = pl.ds(k * RC, RC)

            def one(e):
                r_copy(d, e, k).wait_recv()
                own_sum[d, part] += grp_recv[d, e, part].astype(F32)
            loop(1, S, one)
            if d == 0:
                home_recv[q, part] = own_sum[d, part].astype(BF16)
            else:
                home_send[d, part] = own_sum[d, part].astype(BF16)
                h_copy(d, k).start()

    stage_b(0)
    for i in range(Q):
        if i + 1 < Q:
            stage_a(order[i + 1])
        if i == 0:
            for copy in weights:
                copy.wait()
        if i >= 3:
            stage_f(order[i - 2])
        if i >= 2:
            stage_e(order[i - 1])
        stage_c(order[i])
        if i + 1 < Q:
            stage_b(order[i + 1])
    if Q >= 2:
        stage_e(order[Q - 1])
    stage_e(0)
    for d in order[max(1, Q - 2):]:
        stage_f(d)
    stage_f(0)

    for d in order[1:]:
        for k in range(K):
            h_copy(d, k).wait_recv()
    mixed = jnp.dot(unpack[...], home_recv[...].reshape(Q * R, H), preferred_element_type=F32)
    squares = jnp.sum(mixed * mixed, axis=1, keepdims=True)
    sq_send[...] = jnp.broadcast_to(squares, sq_send.shape)
    sq_copy = remote(sq_send, sq_recv, q_ss, q_rs, at(me, 1 - c))
    sq_copy.start()
    for d in range(Q):
        loop(1 if d == 0 else 0, S, lambda e: gate_copy(d, e).wait_send())
        for k in range(K):
            if d > 0:
                z_copy(d, k).wait_send()
                h_copy(d, k).wait_send()

            def sent(e):
                x_copy(d, e, k).wait_send()
                r_copy(d, e, k).wait_send()
            loop(1, S, sent)
            loop(0, S, lambda e: t_copy(d, e, k).wait_send())
    sq_copy.wait()
    total = squares + sq_recv[:, 0:1]
    out_ref[...] = (mixed * lax.rsqrt(total / width + EPS) * out_gain_ref[...]).astype(BF16)


def body(tokens, in_gain, routing, gate_prob, w_gate, w_up, w_down, out_gain):
    N = lax.axis_size("ep")
    L, D, F = w_gate.shape
    tok, top = routing.shape
    H = out_gain.shape[0]
    group_width = L * N // GROUPS
    cap = max(2, tok * top // (2 * group_width))
    R = min(tok, group_width * cap // top)
    R = -(-R // 16) * 16
    Q, S = GROUPS, N // GROUPS
    lanes = -(-R // 128) * 128
    gate_rows = -(-group_width // 8) * 8
    pair = 2 if S % 2 == 0 else 1
    vmem = pl.BlockSpec(memory_space=pltpu.VMEM)
    hbm = pl.BlockSpec(memory_space=pl.ANY)
    dma = pltpu.SemaphoreType.DMA
    return pl.pallas_call(
        functools.partial(kernel, Q, S, R),
        out_shape=jax.ShapeDtypeStruct((tok, H), BF16),
        in_specs=[vmem] * 4 + [hbm] * 4,
        out_specs=vmem,
        scratch_shapes=[
            pltpu.VMEM((tok, D), BF16),
            pltpu.VMEM((Q, R, H), BF16),
            pltpu.VMEM((Q, S, 2, R, H), BF16),
            pltpu.VMEM((tok, Q * R), BF16),
            pltpu.VMEM((Q, gate_rows, lanes), F32),
            pltpu.VMEM((N, gate_rows, lanes), F32),
            pltpu.VMEM((L, D, F), BF16),
            pltpu.VMEM((L, D, F), BF16),
            pltpu.VMEM((L, F, D), BF16),
            pltpu.VMEM((pair * R, L * F), BF16),
            pltpu.VMEM((2, S, R, H), F32),
            pltpu.VMEM((Q, S, R, H), BF16),
            pltpu.VMEM((Q, S, R, H), BF16),
            pltpu.VMEM((Q, R, H), F32),
            pltpu.VMEM((Q, S, R, H), BF16),
            pltpu.VMEM((Q, R, H), BF16),
            pltpu.VMEM((Q, R, H), BF16),
            pltpu.VMEM((tok, 128), F32),
            pltpu.VMEM((tok, 128), F32),
            dma, dma((3, L)), dma((Q, S)), dma((Q, S)), dma((Q, CHUNKS)), dma((Q, CHUNKS)),
            dma((Q, S, CHUNKS)), dma((Q, S, CHUNKS)), dma((Q, S, CHUNKS)), dma((Q, S, CHUNKS)),
            dma((Q,)), dma((Q,)), dma((Q, S, CHUNKS)), dma((Q, S, CHUNKS)), dma((Q, CHUNKS)), dma((Q, CHUNKS)),
            dma, dma,
        ],
        compiler_params=pltpu.CompilerParams(
            collective_id=0, has_side_effects=True, vmem_limit_bytes=64 * 1000 * 1000
        ),
    )(routing.T, gate_prob.T, in_gain.reshape(1, D), out_gain.reshape(1, H), tokens, w_gate, w_up, w_down)


def solution(mesh):
    placed = (
        P(("grp", "ep"), None),
        P(),
        P(("grp", "ep"), None),
        P(("grp", "ep"), None),
        P("ep", None, "tp"),
        P("ep", None, "tp"),
        P("ep", "tp", None),
        P("tp"),
    )
    return jax.shard_map(
        body, mesh=mesh, in_specs=placed, out_specs=P(("grp", "ep"), "tp"), check_vma=False
    )
```
